32 devices in a mesh: ep: 8 (over z, y), tp: 4 (over x, core).
Axes of the slice: x: 2, y: 2, z: 4, core: 2. Of those that a mesh axis runs over, the one named last changes fastest.
Arguments:
- queries: bfloat16 [4096, 512], P('ep', 'tp'), may hold values from -6 to 6
- key_rows: bfloat16 [4096, 512], P('ep', 'tp'), may hold values from -6 to 6
- value_rows: bfloat16 [4096, 1024], P('ep', 'tp'), may hold values from -6 to 6
- forget_gate_input: bfloat16 [4096, 512], P('ep', 'tp'), may hold values from -6 to 6
- channel_decay_rate: float32 [512], P('tp'), may hold values from 0 to 1, as said below
- position_decay_factor: float32 [4096], P('ep'), may hold values from 0 to 3, as said below
- extra_log_decay: float32 [4096, 8], P('ep', 'tp'), may hold values from -1 to 0, as said below
- head_norm_gain: float32 [8, 128], P('tp'), may hold values from 0.1 to 1.9
- output_projection_weight: bfloat16 [1024, 2048], P('tp'), may hold values from -0.1875 to 0.1875
- expert_input_rows: bfloat16 [2048, 2048], P('ep'), may hold values from -6 to 6
- expert_norm_gain: float32 [2048], replicated, may hold values from 0.1 to 1.9
- routes: int32 [2048, 2], P('ep'), may hold values from 0 to 7, all different within a row; in each aligned block of 256 rows (0 to 255, 256 to 511, ...) at most 128 rows name the same one
- chosen_expert_weights: float32 [2048, 2], P('ep'), may hold values from 0.2 to 1
- expert_gate_weight: bfloat16 [8, 2048, 3072], P('ep', None, 'tp'), may hold values from -0.125 to 0.125
- expert_up_weight: bfloat16 [8, 2048, 3072], P('ep', None, 'tp'), may hold values from -0.125 to 0.125
- expert_down_weight: bfloat16 [8, 3072, 2048], P('ep', 'tp'), may hold values from -0.109375 to 0.109375
Outputs:
- token_mixer_output: bfloat16 [4096, 2048], P(('ep', 'tp'))
- moe_out: bfloat16 [2048, 2048], P('ep', 'tp')
The draws below stay inside these ranges and needn't reach their ends.
Inputs may be any that keep to these rules, and one draw needn't show every extreme that they name: `routes`: within the rows of one device no expert is named by more than 128 of the choices, a bound that some block reaches; the 2 experts of a token differ. `channel_decay_rate`: Positive. `position_decay_factor`: Positive. `extra_log_decay`: zero or negative.
All inputs are finite; a program needn't handle non-finite values.
Results may differ from the reference program's by a relative error of at most 0.019.
Values may be sent and summed in bfloat16 or wider, within the bound.
A program may use at most 128 MiB of HBM per device.

```python
import math
import jax
import jax.numpy as jnp
import numpy as np
from jax import lax

D = 2048
HEAD_TOTAL = 8
KEY_CHANNELS = 64
VALUE_DIM = 128
SPAN = 64
FF = 3072
TOPK = 2
TOK_EP = 512
TOK_MOE = 256
TOKENS_MIX = 4096
TOKENS_MOE = 2048
EXPERTS = 8
CAPACITY = 128
N_EP = 8
N_TP = 4


def draw_channel_decay_rate(key, part):
    keys_list = jax.random.split(jax.random.fold_in(key, 11), 3)
    slow_share = 0.5
    slow_heads = jax.random.uniform(keys_list[0], (HEAD_TOTAL,)) < slow_share
    slow_rates = jnp.exp(jax.random.uniform(keys_list[1], (HEAD_TOTAL, KEY_CHANNELS), minval=jnp.log(0.2), maxval=0.0)) / TOKENS_MIX
    fast_rates = jnp.exp(jax.random.uniform(keys_list[2], (HEAD_TOTAL, KEY_CHANNELS), minval=jnp.log(0.03), maxval=jnp.log(0.12)))
    return jnp.where(slow_heads[:, None], slow_rates, fast_rates).reshape(HEAD_TOTAL * KEY_CHANNELS).astype(jnp.float32)


def draw_position_decay_factor(key, part):
    block_key, position_key = jax.random.split(jax.random.fold_in(key, 23))
    blocks = TOKENS_MIX // TOK_EP
    block_scale = jnp.exp(jax.random.uniform(block_key, (blocks,), minval=-0.7, maxval=0.7))
    jitter = jnp.exp(jax.random.uniform(position_key, (TOKENS_MIX,), minval=-0.35, maxval=0.35))
    return (jnp.repeat(block_scale, TOK_EP) * jitter).astype(jnp.float32)


def draw_extra_log_decay(key, part):
    where_key, depth_key = jax.random.split(jax.random.fold_in(key, 37))
    struck = jax.random.uniform(where_key, (TOKENS_MIX, HEAD_TOTAL)) < 3.0 / TOKENS_MIX
    depth = jax.random.uniform(depth_key, (TOKENS_MIX, HEAD_TOTAL), minval=-0.6, maxval=-0.2)
    return jnp.where(struck, depth, 0.0).astype(jnp.float32)


def steps_of(rng, extent, cuts, low, largest):
    def one(position, blocks):
        heights = jax.random.uniform(jax.random.fold_in(jax.random.fold_in(rng, 6), position), (blocks,), jnp.float32, low / len(cuts), largest / len(cuts))
        return jnp.repeat(jnp.exp(heights), extent[position] // blocks).reshape((-1,) + (1,) * (len(extent) - position - 1))

    factor_of = one(*cuts[0])
    for cut in cuts[1:]:
        factor_of = factor_of * one(*cut)
    return factor_of


def shared_out(key, own, number, rows, amount, top, reach, lean):
    order = jax.random.permutation(key, amount)
    heavy_load, usual = load_shares(amount, rows * top, reach, lean, True), load_shares(amount, rows * top, reach, lean, False)
    places = jnp.arange(amount)

    def named(tallies, offset_by):
        used = int((tallies > 0).sum())
        fixed = max(1, used // 4)
        moved = fixed + (places - fixed + offset_by * (used - fixed)) % max(1, amount - fixed)
        return jnp.zeros((amount,), jnp.int32).at[order[jnp.where(places < fixed, places, moved)]].set(jnp.asarray(tallies, jnp.int32))

    tallies = jnp.where(number % 4 == 0, named(heavy_load, number // 4), named(usual, number - number // 4 - 1))
    mixed = jax.random.permutation(jax.random.fold_in(own, 3), amount)
    donor, sink = mixed[0:amount // 2 * 2:2], mixed[1:amount // 2 * 2:2]
    room = jnp.minimum(tallies[donor] - 1, reach - tallies[sink]) // 2
    room = jnp.where((donor == order[0]) | (sink == order[0]) | (tallies[sink] == 0), 0, jnp.maximum(room, 0))
    moved = jax.random.randint(jax.random.fold_in(own, 4), (amount // 2,), 0, 1 << 20) % (room + 1)
    tallies = tallies.at[donor].add(-moved).at[sink].add(moved)
    items = jnp.searchsorted(jnp.cumsum(tallies), jnp.arange(rows * top), side="right").astype(jnp.int32)
    grid = items.reshape(top, rows).T
    grid = grid[jax.random.permutation(jax.random.fold_in(own, 1), rows)]
    offset_by = jax.random.randint(jax.random.fold_in(own, 2), (rows, 1), 0, top)
    return jnp.take_along_axis(grid, (jnp.arange(top)[None, :] + offset_by) % top, axis=1)


def load_shares(number_of, total, limit, lean, full):
    loads = [(1 << 20) // math.isqrt(rank ** lean) + 1 for rank in range(1, number_of + 1)]
    largest = limit if full else min(limit, max(-(-total // number_of), total * loads[0] // sum(loads)))
    least = 1 if total - largest >= number_of - 1 else 0
    counts, rest = [largest] + [least] * (number_of - 1), total - largest - least * (number_of - 1)
    while rest > 0:
        free = [i for i in range(1, number_of) if counts[i] < largest] or [i for i in range(1, number_of) if counts[i] < limit]
        pool, budget = sum([loads[i] for i in free]), rest
        for i in free:
            more = min(limit - counts[i], max(1, budget * loads[i] // pool), rest)
            counts[i] = counts[i] + more
            rest = rest - more
    return np.array(counts)


def centred(key, extent, spread, reach, shards=(), kind=jnp.bfloat16):
    result = spread * jax.random.normal(key, extent, jnp.float32)
    if shards:
        result = result * steps_of(key, extent, shards, -0.22, 0.18)
    return jnp.clip(result, -reach, reach).astype(kind)


def setup_inputs(seed: int = 0) -> dict:
    seeds = jax.random.split(jax.random.key(seed), 17)
    queries = centred(seeds[0], (TOKENS_MIX, HEAD_TOTAL * KEY_CHANNELS), 1.0, 6.0, ((0, 8), (1, 4)))
    key_rows = centred(seeds[1], (TOKENS_MIX, HEAD_TOTAL * KEY_CHANNELS), 1.0, 6.0, ((0, 8), (1, 4)))
    value_rows = centred(seeds[2], (TOKENS_MIX, HEAD_TOTAL * VALUE_DIM), 1.0, 6.0, ((0, 8), (1, 4)))
    forget_gate_input = centred(seeds[3], (TOKENS_MIX, HEAD_TOTAL * KEY_CHANNELS), 1.5, 6.0, ((0, 8), (1, 4)))
    channel_decay_rate = draw_channel_decay_rate(jax.random.fold_in(seeds[16], 71), 0)
    position_decay_factor = draw_position_decay_factor(jax.random.fold_in(seeds[16], 71), 0)
    extra_log_decay = draw_extra_log_decay(jax.random.fold_in(seeds[16], 71), 0)
    head_norm_gain = jnp.clip(1.0 + 0.18 * jax.random.normal(seeds[7], (HEAD_TOTAL, VALUE_DIM), jnp.float32), 0.1, 1.9)
    output_projection_weight = centred(seeds[8], (HEAD_TOTAL * VALUE_DIM, D), (HEAD_TOTAL * VALUE_DIM) ** -0.5, 0.1875, ((0, 4),))
    expert_input_rows = centred(seeds[9], (TOKENS_MOE, D), 1.0, 6.0, ((0, 8),))
    expert_norm_gain = jnp.clip(1.0 + 0.18 * jax.random.normal(seeds[10], (D,), jnp.float32), 0.1, 1.9)
    routes_keys = jax.random.split(jax.random.fold_in(seeds[11], 1), TOKENS_MOE // TOK_MOE)
    routes_turns = jax.random.permutation(jax.random.fold_in(seeds[11], 3), TOKENS_MOE // TOK_MOE)
    routes = jax.vmap(lambda own, number: shared_out(jax.random.fold_in(seeds[11], 2), own, number, TOK_MOE, EXPERTS, TOPK, CAPACITY, 1))(routes_keys, routes_turns).reshape((TOKENS_MOE, TOPK))
    chosen_expert_weights = jnp.clip(0.2 + 0.8 * jax.random.uniform(seeds[12], (TOKENS_MOE, TOPK), jnp.float32) ** steps_of(seeds[12], (TOKENS_MOE, TOPK), ((0, 8),), -0.2, 0.2), 0.2, 1.0)
    expert_gate_weight = centred(seeds[13], (EXPERTS, D, FF), D ** -0.5, 0.125, ((0, 8), (2, 4)))
    expert_up_weight = centred(seeds[14], (EXPERTS, D, FF), D ** -0.5, 0.125, ((0, 8), (2, 4)))
    expert_down_weight = centred(seeds[15], (EXPERTS, FF, D), FF ** -0.5, 0.109375, ((0, 8), (1, 4)))
    return dict(queries=queries, key_rows=key_rows, value_rows=value_rows, forget_gate_input=forget_gate_input, channel_decay_rate=channel_decay_rate, position_decay_factor=position_decay_factor, extra_log_decay=extra_log_decay, head_norm_gain=head_norm_gain, output_projection_weight=output_projection_weight, expert_input_rows=expert_input_rows, expert_norm_gain=expert_norm_gain, routes=routes, chosen_expert_weights=chosen_expert_weights, expert_gate_weight=expert_gate_weight, expert_up_weight=expert_up_weight, expert_down_weight=expert_down_weight)


highest_precision = lax.Precision.HIGHEST
norm_eps = 1e-06

def gla_blocks(query_single, key_float, value_float, decay_logarithm, span_rows):
    length, head_count, key_width = query_single.shape
    value_width = value_float.shape[-1]
    block_count = length // span_rows

    def blocked(tensor):
        return tensor.reshape(block_count, span_rows, head_count, tensor.shape[-1])
    causal = (jnp.arange(span_rows)[:, None] >= jnp.arange(span_rows)[None, :])[:, :, None, None]

    def advance(carried_state, pieces):
        block_queries, block_keys, block_values, gate_block = pieces
        cumulative_decay = jnp.cumsum(gate_block, axis=0)
        log_gaps = cumulative_decay[:, None] - cumulative_decay[None, :]
        decays = jnp.exp(jnp.where(causal, log_gaps, -jnp.inf))
        scores = lax.optimization_barrier(jnp.sum(block_queries[:, None] * block_keys[None, :] * decays, axis=-1))
        final_output = jnp.einsum('ijh,jhv->ihv', scores, block_values, precision=highest_precision)
        final_output = final_output + jnp.einsum('nwt,wto->nwo', block_queries * jnp.exp(cumulative_decay), carried_state, precision=highest_precision)
        final_log_decay = cumulative_decay[-1]
        carried_state = jnp.exp(final_log_decay)[:, :, None] * carried_state + jnp.einsum('ygc,yga->gca', block_keys * jnp.exp(final_log_decay[None] - cumulative_decay), block_values, precision=highest_precision)
        return (carried_state, final_output)
    start_state = jnp.zeros((head_count, key_width, value_width), jnp.float32)
    carried_state, outputs = lax.scan(advance, start_state, (blocked(query_single), blocked(key_float), blocked(value_float), blocked(decay_logarithm)))
    return (outputs.reshape(length, head_count, value_width), carried_state)

def reference_mixer(queries, key_rows, value_rows, forget_gate_input, channel_decay_rate, position_decay_factor, extra_log_decay, head_norm_gain, output_projection_weight):
    length = queries.shape[0]
    query_single = queries.astype(jnp.float32).reshape(length, HEAD_TOTAL, KEY_CHANNELS)
    key_float = key_rows.astype(jnp.float32).reshape(length, HEAD_TOTAL, KEY_CHANNELS)
    value_float = value_rows.astype(jnp.float32).reshape(length, HEAD_TOTAL, VALUE_DIM)
    gate_logarithm = jax.nn.log_sigmoid(forget_gate_input.astype(jnp.float32)).reshape(length, HEAD_TOTAL, KEY_CHANNELS)
    decay_logarithm = gate_logarithm * channel_decay_rate.reshape(HEAD_TOTAL, KEY_CHANNELS)[None] * position_decay_factor[:, None, None] + extra_log_decay[:, :, None]
    mixed_out, unused = gla_blocks(query_single, key_float, value_float, decay_logarithm, SPAN)
    scale = lax.rsqrt(lax.optimization_barrier(jnp.mean(mixed_out * mixed_out, axis=-1, keepdims=True)) + norm_eps)
    head_normed = (mixed_out * scale * head_norm_gain[None]).astype(jnp.bfloat16).reshape(length, HEAD_TOTAL * VALUE_DIM)
    group_width = HEAD_TOTAL * VALUE_DIM // N_TP
    running = jnp.zeros((length, D), jnp.float32)
    for member in range(N_TP):
        partial_value = jnp.dot(head_normed[:, member * group_width:(member + 1) * group_width], output_projection_weight[member * group_width:(member + 1) * group_width], preferred_element_type=jnp.float32).astype(jnp.bfloat16)
        running = running + lax.optimization_barrier(partial_value).astype(jnp.float32)
    return running.astype(jnp.bfloat16)

def expert_reference(expert_input_rows, expert_norm_gain, routes, chosen_expert_weights, expert_gate_weight, expert_up_weight, expert_down_weight):
    rows_float = expert_input_rows.astype(jnp.float32)
    scaled = rows_float * lax.rsqrt(lax.optimization_barrier(jnp.mean(rows_float * rows_float, axis=-1, keepdims=True)) + norm_eps)
    moe_normed = (scaled * expert_norm_gain[None]).astype(jnp.bfloat16)
    flat_routes = routes.reshape(-1)
    flat_weights = chosen_expert_weights.reshape(-1)
    slot_total = N_EP * CAPACITY
    group_width = FF // N_TP

    def one_expert(accumulator, inputs):
        gate_weight, up_weight, down_weight, expert_id = inputs
        routed_here = flat_routes == expert_id
        picked = jnp.nonzero(routed_here, size=slot_total, fill_value=0)[0].astype(jnp.int32)
        live_slot = (jnp.arange(slot_total, dtype=jnp.int32) < jnp.sum(routed_here.astype(jnp.int32))).astype(jnp.float32)
        token_rows = (picked // TOPK).astype(jnp.int32)
        chosen = moe_normed[token_rows]
        gate_sum = jnp.dot(chosen, gate_weight, preferred_element_type=jnp.float32)
        up_sum = jnp.dot(chosen, up_weight, preferred_element_type=jnp.float32)
        hidden = (jax.nn.silu(gate_sum) * up_sum).astype(jnp.bfloat16)
        running = jnp.zeros((slot_total, D), jnp.float32)
        for member in range(N_TP):
            partial_value = jnp.dot(hidden[:, member * group_width:(member + 1) * group_width], down_weight[member * group_width:(member + 1) * group_width], preferred_element_type=jnp.float32).astype(jnp.bfloat16)
            running = running + lax.optimization_barrier(partial_value).astype(jnp.float32)
        expert_result = lax.optimization_barrier(running.astype(jnp.bfloat16)).astype(jnp.float32)
        weighted = expert_result * (flat_weights[picked] * live_slot)[:, None]
        return (accumulator.at[token_rows].add(weighted), None)
    empty_sum = jnp.zeros((TOKENS_MOE, D), jnp.float32)
    combined, unused = lax.scan(one_expert, empty_sum, (expert_gate_weight, expert_up_weight, expert_down_weight, jnp.arange(EXPERTS, dtype=jnp.int32)))
    return combined.astype(jnp.bfloat16)

def reference(queries, key_rows, value_rows, forget_gate_input, channel_decay_rate, position_decay_factor, extra_log_decay, head_norm_gain, output_projection_weight, expert_input_rows, expert_norm_gain, routes, chosen_expert_weights, expert_gate_weight, expert_up_weight, expert_down_weight):
    token_mixer_output = reference_mixer(queries, key_rows, value_rows, forget_gate_input, channel_decay_rate, position_decay_factor, extra_log_decay, head_norm_gain, output_projection_weight)
    moe_out = expert_reference(expert_input_rows, expert_norm_gain, routes, chosen_expert_weights, expert_gate_weight, expert_up_weight, expert_down_weight)
    return (token_mixer_output, moe_out)
```

```python
import functools

import jax
import jax.numpy as jnp
from jax import lax
from jax.experimental import pallas as pl
from jax.experimental.pallas import tpu as pltpu
from jax.sharding import PartitionSpec as P

EPS = 1e-06
CHUNK = 128
GROUP_ROWS = 256
BF = jnp.bfloat16
F32 = jnp.float32
MESH = pl.DeviceIdType.MESH


def flip(a, b, size):
    total = 0
    bit = 1
    while bit < size:
        total = total + ((a // bit) % 2 + (b // bit) % 2) % 2 * bit
        bit *= 2
    return total


def dot(a, b, dims=((1,), (0,))):
    return lax.dot_general(a, b, (dims, ((), ())), preferred_element_type=F32)


def iota(shape, dim):
    return lax.broadcasted_iota(jnp.int32, shape, dim)


def level_sums(half):
    i, t = iota((CHUNK, CHUNK), 0), iota((CHUNK, CHUNK), 1)
    step = 2 * half
    same = (i // step) == (t // step)
    upper_i, upper_t = (i % step) >= half, (t % step) >= half
    return same & ((upper_i & upper_t & (t <= i)) | (~upper_i & ~upper_t & (t > i)))


def level_pairs(half):
    i, j = iota((CHUNK, CHUNK), 0), iota((CHUNK, CHUNK), 1)
    step = 2 * half
    return ((i // step) == (j // step)) & ((i % step) >= half) & ((j % step) < half)


def kernel(
    ep, tp,
    q_ref, k_ref, v_ref, f_ref, rate_ref, aux_ref, hgain_ref, x_ref, xgain_ref, routes_ref, w_ref,
    wo_hbm, wg_hbm, wu_hbm, wd_hbm,
    out1, out2,
    disp, recv, psend, pkeep, precv, xsum, xrecv, fin, ret, hot,
    sums, oloc, qin, state, ssend, srecv, dsend, drecv, hn,
    msend, mkeep, mprecv, mxsum, mxrecv,
    wo, wg, wu, wd,
    ep_s, ep_r, x_s, x_r, p_s, p_r, r_s, r_r,
    fp_s, fp_r, fx_s, fx_r, b_s, b_r,
    st_s, st_r, dc_s, dc_r,
    mp_s, mp_r, mx_s, mx_r, w_s,
):
    me, col = lax.axis_index("ep"), lax.axis_index("tp")
    partner = col + 1 - 2 * (col % 2)
    across = (col + 2) % tp
    diagonal = (partner + 2) % tp
    tokens, quarter = out2.shape
    slots = disp.shape[0]
    cap = slots // ep
    group = min(GROUP_ROWS, slots)
    per_group = group // cap
    groups = slots // group
    length = q_ref.shape[0]
    chunks = length // CHUNK
    values = v_ref.shape[1] // 2
    rows_out = out1.shape[0]

    def remote(src, dst, s, r, **where):
        return pltpu.make_async_remote_copy(
            src_ref=src, dst_ref=dst, send_sem=s, recv_sem=r, device_id=where, device_id_type=MESH
        )

    loads = [
        pltpu.make_async_copy(a, b, w_s.at[n])
        for n, (a, b) in enumerate(((wg_hbm.at[0], wg), (wu_hbm.at[0], wu), (wd_hbm.at[0], wd), (wo_hbm, wo)))
    ]
    for load in loads:
        load.start()

    barrier = pltpu.get_barrier_semaphore()
    for d in range(1, ep):
        pl.semaphore_signal(barrier, inc=1, device_id={"ep": flip(me, d, ep)}, device_id_type=MESH)
    for peer in (partner, across):
        pl.semaphore_signal(barrier, inc=1, device_id={"tp": peer}, device_id_type=MESH)

    lower = (iota((tokens, tokens), 0) <= iota((tokens, tokens), 1)).astype(BF)
    expert = iota((ep, tokens), 0)
    first_slot = flip(expert, me, ep) * cap - 1
    before = jnp.zeros((ep, 1), F32)
    for choice in range(2):
        named = expert == routes_ref[choice : choice + 1, :]
        rank = dot(named.astype(F32).astype(BF), lower) + before
        place = jnp.sum(jnp.where(named, rank.astype(jnp.int32) + first_slot, 0), axis=0, keepdims=True)
        before = rank[:, tokens - 1 : tokens]
        hot[choice] = (iota((slots, tokens), 0) == place).astype(F32).astype(BF)
    rows = x_ref[...].astype(F32)
    scale = lax.rsqrt(jnp.mean(rows * rows, axis=-1, keepdims=True) + EPS)
    columns = pl.ds(pl.multiple_of(col * quarter, quarter), quarter)
    normed = (x_ref[:, columns].astype(F32) * scale * xgain_ref[:, columns]).astype(BF)
    for g in range(groups):
        span = pl.ds(g * group, group)
        disp[span, :] = dot(hot[0, span, :] + hot[1, span, :], normed).astype(BF)
    recv[col, pl.ds(0, cap), :] = disp[0:cap, :]

    pl.semaphore_wait(barrier, ep + 1)

    def block(d):
        return pl.ds(d * cap, cap)

    def to_expert(d):
        return remote(disp.at[block(d)], recv.at[col, block(d)], ep_s.at[d], ep_r.at[d], ep=flip(me, d, ep))

    def over(d):
        return remote(recv.at[col, block(d)], recv.at[col, block(d)], x_s.at[d], x_r.at[d], tp=across)

    def over_in(d):
        return remote(recv.at[across, block(d)], recv.at[across, block(d)], x_s.at[d], x_r.at[d], tp=across)

    def beside(d):
        return remote(recv.at[col, block(d)], recv.at[col, block(d)], p_s.at[d], p_r.at[d], tp=partner)

    def beside_in(d):
        return remote(recv.at[partner, block(d)], recv.at[partner, block(d)], p_s.at[d], p_r.at[d], tp=partner)

    def relay(d):
        return remote(recv.at[across, block(d)], recv.at[across, block(d)], r_s.at[d], r_r.at[d], tp=partner)

    def relay_in(d):
        return remote(recv.at[diagonal, block(d)], recv.at[diagonal, block(d)], r_s.at[d], r_r.at[d], tp=partner)

    for d in range(1, ep):
        to_expert(d).start()

    def forward(d):
        if d:
            to_expert(d).wait_recv()
        over(d).start()
        beside(d).start()

    def pass_on(d):
        over_in(d).wait_recv()
        relay(d).start()

    forward(0)

    halves = []
    half = CHUNK // 2
    while half:
        halves.append(half)
        half //= 2
    count = len(halves)
    for n, h in enumerate(halves):
        sums[n * CHUNK : (n + 1) * CHUNK, :] = level_sums(h).astype(F32).astype(BF)
    ci, ct = iota((CHUNK, CHUNK), 0), iota((CHUNK, CHUNK), 1)
    sums[count * CHUNK : (count + 1) * CHUNK, :] = (ct <= ci).astype(F32).astype(BF)
    sums[(count + 1) * CHUNK : (count + 2) * CHUNK, :] = (ct > ci).astype(F32).astype(BF)
    width = q_ref.shape[1]
    lane = iota((CHUNK, width), 1)
    head_of = [(lane < width // 2).astype(F32), (lane >= width // 2).astype(F32)]
    ones = jnp.ones((CHUNK, values), BF)
    state[...] = jnp.zeros_like(state)
    so_far = [jnp.zeros((1, width), F32)]

    def recur(c):
        at = pl.ds(c * CHUNK, CHUNK)
        gate = f_ref[at, :].astype(F32)
        log_gate = jnp.minimum(gate, 0.0) - jnp.log1p(jnp.exp(-jnp.abs(gate)))
        extra = jnp.where(lane < width // 2, aux_ref[at, 1:2], aux_ref[at, 2:3])
        decay = log_gate * rate_ref[...] * aux_ref[at, 0:1] + extra
        high = decay.astype(BF)
        low = (decay - high.astype(F32)).astype(BF)
        logs = dot(sums[...], high) + dot(sums[...], low)
        q, k = q_ref[at, :].astype(F32), k_ref[at, :].astype(F32)

        def both(a):
            return jnp.concatenate([a * head_of[0], a * head_of[1]], axis=0).astype(BF)

        def scores(a, b, mask):
            s = dot(both(a), b.astype(BF), ((1,), (1,)))
            return [jnp.where(mask, s[:CHUNK], 0.0), jnp.where(mask, s[CHUNK:], 0.0)]

        total = scores(q, k, ci == ct)
        for n, h in enumerate(halves):
            e = jnp.exp(logs[n * CHUNK : (n + 1) * CHUNK])
            part = scores(q * e, k * e, level_pairs(h))
            total = [total[0] + part[0], total[1] + part[1]]
        prefix = logs[count * CHUNK : (count + 1) * CHUNK]
        suffix = logs[(count + 1) * CHUNK :]
        held = state[...].astype(BF)
        carried = dot(both(q * jnp.exp(prefix)), held)
        key_end = k * jnp.exp(suffix)
        new = jnp.exp(dot(high, ones, ((0,), (0,))) + dot(low, ones, ((0,), (0,)))) * state[...]
        for head in range(2):
            v = v_ref[at, head * values : (head + 1) * values]
            oloc[at, head * values : (head + 1) * values] = (
                dot(total[head].astype(BF), v) + carried[head * CHUNK : (head + 1) * CHUNK]
            )
            new = new + dot((key_end * head_of[head]).astype(BF), v, ((0,), (0,)))
        state[...] = new
        qin[at, :] = (q * jnp.exp(prefix + so_far[0])).astype(BF)
        so_far[0] = so_far[0] + prefix[CHUNK - 1 : CHUNK]

    forwarded, passed = 1, 0
    for c in range(chunks):
        recur(c)
        if c and forwarded < min(ep, 2 * per_group):
            forward(forwarded)
            forwarded += 1
            pass_on(passed)
            passed += 1

    ssend[...] = state[...].astype(BF)
    dsend[...] = jnp.where(iota(dsend.shape, 0) == 0, so_far[0], 0.0)

    def state_out(e):
        return (
            remote(ssend, srecv.at[me], st_s.at[e], st_r.at[me], ep=e),
            remote(dsend, drecv.at[me], dc_s.at[e], dc_r.at[me], ep=e),
        )

    def state_in(e):
        return (
            remote(ssend, srecv.at[e], st_s.at[e], st_r.at[e], ep=e),
            remote(dsend, drecv.at[e], dc_s.at[e], dc_r.at[e], ep=e),
        )

    for e in range(ep):
        @pl.when(e > me)
        def _():
            for copy in state_out(e):
                copy.start()

    def part_copy(g, n):
        at = pl.ds(g * group, group)
        return remote(psend.at[n, at], precv.at[n, at], fp_s.at[n, g], fp_r.at[n, g], tp=partner)

    def sum_copy(g):
        at = pl.ds(g * group, group)
        return remote(xsum.at[at], xrecv.at[at], fx_s.at[g], fx_r.at[g], tp=across)

    def back(d):
        return remote(fin.at[block(d)], ret.at[block(d)], b_s.at[d], b_r.at[d], ep=flip(me, d, ep))

    progress = [forwarded, passed]

    def advance(until, relayed):
        while progress[0] < min(until, ep):
            forward(progress[0])
            progress[0] += 1
        while progress[1] < min(relayed, ep):
            pass_on(progress[1])
            progress[1] += 1

    def experts(g):
        at = pl.ds(g * group, group)
        gate = up = None
        for n in range(tp):
            inner = slice(n * quarter, (n + 1) * quarter)
            piece = recv[n, at, :]
            a, b = dot(piece, wg[inner, :]), dot(piece, wu[inner, :])
            gate, up = (a, b) if gate is None else (gate + a, up + b)
        hidden = (gate * (1.0 / (1.0 + jnp.exp(-gate))) * up).astype(BF)

        def piece_of(c):
            return dot(hidden, wd[:, pl.ds(pl.multiple_of(c * quarter, quarter), quarter)]).astype(BF)

        for n, c in enumerate((diagonal, partner)):
            psend[n, at, :] = piece_of(c)
            part_copy(g, n).start()
        for n, c in enumerate((across, col)):
            pkeep[n, at, :] = piece_of(c)

    def pair(g):
        at = pl.ds(g * group, group)
        part_copy(g, 0).wait_recv()
        xsum[at, :] = (pkeep[0, at, :].astype(F32) + precv[0, at, :].astype(F32)).astype(BF)
        sum_copy(g).start()

    def finish(g):
        at = pl.ds(g * group, group)
        part_copy(g, 1).wait_recv()
        sum_copy(g).wait_recv()
        value = (
            pkeep[1, at, :].astype(F32) + precv[1, at, :].astype(F32) + xrecv[at, :].astype(F32)
        ).astype(BF)
        fin[at, :] = value
        if g == 0:
            ret[0:cap, :] = value[0:cap]
        for d in range(max(1, g * per_group), (g + 1) * per_group):
            back(d).start()

    def mixer_copy(n):
        return remote(msend.at[n], mprecv.at[n], mp_s.at[n], mp_r.at[n], tp=partner)

    def mixer_sum():
        return remote(mxsum, mxrecv, mx_s.at[0], mx_r.at[0], tp=across)

    def mixer_project():
        state[...] = jnp.zeros_like(state)
        for e in range(ep - 1):
            @pl.when(e < me)
            def _():
                for copy in state_in(e):
                    copy.wait_recv()
                logs = lax.dot_general(
                    drecv[e], jnp.ones(drecv.shape[1:2] + (values,), F32), (((0,), (0,)), ((), ())),
                    precision=lax.Precision.HIGHEST, preferred_element_type=F32,
                )
                state[...] = jnp.exp(logs) * state[...] + srecv[e].astype(F32)
        held = state[...]
        row = iota(held.shape, 0)
        for head in range(2):
            mine = (row < width // 2) if head == 0 else (row >= width // 2)
            cols = slice(head * values, (head + 1) * values)
            o = oloc[:, cols] + dot(qin[...], jnp.where(mine, held, 0.0).astype(BF))
            s = lax.rsqrt(jnp.mean(o * o, axis=-1, keepdims=True) + EPS)
            hn[:, cols] = (o * s * hgain_ref[head : head + 1, :]).astype(BF)
        loads[3].wait()

        def piece_of(r):
            return dot(hn[pl.ds(pl.multiple_of(r * rows_out, rows_out), rows_out), :], wo[...]).astype(BF)

        for n, r in enumerate((diagonal, partner)):
            msend[n] = piece_of(r)
            mixer_copy(n).start()
        for n, r in enumerate((across, col)):
            mkeep[n] = piece_of(r)

    def mixer_pair():
        mixer_copy(0).wait_recv()
        mxsum[...] = (mkeep[0].astype(F32) + mprecv[0].astype(F32)).astype(BF)
        mixer_sum().start()

    for load in loads[:3]:
        load.wait()
    for g in range(groups):
        first, last = g * per_group, (g + 1) * per_group
        advance(last, last)
        for d in range(first, last):
            beside_in(d).wait_recv()
            relay_in(d).wait_recv()
        experts(g)
        advance(last + per_group, last)
        pair(g)
        if g == min(1, groups - 1):
            mixer_project()
        if g == min(2, groups - 1):
            mixer_pair()
        if g:
            finish(g - 1)
    finish(groups - 1)

    mixer_copy(1).wait_recv()
    mixer_sum().wait_recv()
    out1[...] = (mkeep[1].astype(F32) + mprecv[1].astype(F32) + mxrecv[...].astype(F32)).astype(BF)

    for d in range(1, ep):
        back(d).wait_recv()
    picked = [dot(hot[choice], ret[...], ((0,), (0,))) for choice in range(2)]
    out2[...] = (picked[0] * w_ref[:, 0:1] + picked[1] * w_ref[:, 1:2]).astype(BF)

    for d in range(ep):
        if d:
            to_expert(d).wait_send()
            back(d).wait_send()
        over(d).wait_send()
        beside(d).wait_send()
        relay(d).wait_send()
    for g in range(groups):
        for n in range(2):
            part_copy(g, n).wait_send()
        sum_copy(g).wait_send()
    for n in range(2):
        mixer_copy(n).wait_send()
    mixer_sum().wait_send()
    for e in range(ep):
        @pl.when(e > me)
        def _():
            for copy in state_out(e):
                copy.wait_send()


def body(q, k, v, f, rate, factor, extra, head_gain, wo, x, x_gain, routes, weights, wg, wu, wd):
    ep, tp = lax.axis_size("ep"), lax.axis_size("tp")
    length, width = q.shape
    values = head_gain.shape[1]
    tokens, model = x.shape
    quarter = model // tp
    hidden = wg.shape[2]
    cap = 4 * tokens // ep
    slots = ep * cap
    group = min(GROUP_ROWS, slots)
    groups = slots // group
    rows_out = length // tp
    aux = jnp.concatenate([factor[:, None], extra], axis=1)
    vm, hbm = pl.BlockSpec(memory_space=pltpu.VMEM), pl.BlockSpec(memory_space=pl.ANY)
    V = pltpu.VMEM
    sem = lambda *shape: pltpu.SemaphoreType.DMA(shape)
    levels = CHUNK.bit_length() + 1
    return pl.pallas_call(
        functools.partial(kernel, ep, tp),
        out_shape=(
            jax.ShapeDtypeStruct((rows_out, model), BF),
            jax.ShapeDtypeStruct((tokens, quarter), BF),
        ),
        in_specs=[vm] * 11 + [hbm] * 4,
        out_specs=(vm, vm),
        scratch_shapes=[
            V((slots, quarter), BF), V((tp, slots, quarter), BF), V((2, slots, quarter), BF),
            V((2, slots, quarter), BF), V((2, slots, quarter), BF), V((slots, quarter), BF),
            V((slots, quarter), BF), V((slots, quarter), BF), V((slots, quarter), BF),
            V((2, slots, tokens), BF),
            V((levels * CHUNK, CHUNK), BF), V((length, 2 * values), F32), V((length, width), BF),
            V((width, values), F32), V((width, values), BF), V((ep, width, values), BF),
            V((8, width), F32), V((ep, 8, width), F32), V((length, 2 * values), BF),
            V((2, rows_out, model), BF), V((2, rows_out, model), BF), V((2, rows_out, model), BF),
            V((rows_out, model), BF), V((rows_out, model), BF),
            V(wo.shape, BF), V(wg.shape[1:], BF), V(wu.shape[1:], BF), V(wd.shape[1:], BF),
            sem(ep), sem(ep), sem(ep), sem(ep), sem(ep), sem(ep), sem(ep), sem(ep),
            sem(2, groups), sem(2, groups), sem(groups), sem(groups), sem(ep), sem(ep),
            sem(ep), sem(ep), sem(ep), sem(ep),
            sem(2), sem(2), sem(1), sem(1), sem(4),
        ],
        compiler_params=pltpu.CompilerParams(
            collective_id=0, has_side_effects=True, vmem_limit_bytes=60 * 1024 * 1024
        ),
    )(q, k, v, f, rate[None], aux, head_gain, x, x_gain[None], routes.T, weights, wo, wg, wu, wd)


def solution(mesh):
    return jax.shard_map(
        body,
        mesh=mesh,
        in_specs=(
            P("ep", "tp"),
            P("ep", "tp"),
            P("ep", "tp"),
            P("ep", "tp"),
            P("tp"),
            P("ep"),
            P("ep", "tp"),
            P("tp", None),
            P("tp", None),
            P("ep", None),
            P(),
            P("ep", None),
            P("ep", None),
            P("ep", None, "tp"),
            P("ep", None, "tp"),
            P("ep", "tp", None),
        ),
        out_specs=(P(("ep", "tp"), None), P("ep", "tp")),
        check_vma=False,
    )
```

```python
import functools

import jax
import jax.numpy as jnp
from jax import lax
from jax.experimental import pallas as pl
from jax.experimental.pallas import tpu as pltpu
from jax.sharding import PartitionSpec as P

EPS = 1e-06
CHUNK = 128
GROUP_ROWS = 256
BF = jnp.bfloat16
F32 = jnp.float32
MESH = pl.DeviceIdType.MESH


def flip(a, b, size):
    total = 0
    bit = 1
    while bit < size:
        total = total + ((a // bit) % 2 + (b // bit) % 2) % 2 * bit
        bit *= 2
    return total


def dot(a, b, dims=((1,), (0,))):
    return lax.dot_general(a, b, (dims, ((), ())), preferred_element_type=F32)


def iota(shape, dim):
    return lax.broadcasted_iota(jnp.int32, shape, dim)


def level_sums(half):
    i, t = iota((CHUNK, CHUNK), 0), iota((CHUNK, CHUNK), 1)
    step = 2 * half
    same = (i // step) == (t // step)
    upper_i, upper_t = (i % step) >= half, (t % step) >= half
    return same & ((upper_i & upper_t & (t <= i)) | (~upper_i & ~upper_t & (t > i)))


def level_pairs(half):
    i, j = iota((CHUNK, CHUNK), 0), iota((CHUNK, CHUNK), 1)
    step = 2 * half
    return ((i // step) == (j // step)) & ((i % step) >= half) & ((j % step) < half)


def kernel(
    ep, tp,
    q_ref, k_ref, v_ref, f_ref, rate_ref, aux_ref, hgain_ref, x_ref, xgain_ref, routes_ref, w_ref,
    wo_hbm, wg_hbm, wu_hbm, wd_hbm,
    out1, out2,
    disp, recv, psend, pkeep, precv, xsum, xrecv, fin, ret, hot,
    sums, oloc, qin, state, ssend, srecv, dsend, drecv, hn,
    msend, mkeep, mprecv, mxsum, mxrecv,
    wo, wg, wu, wd,
    ep_s, ep_r, x_s, x_r, p_s, p_r, r_s, r_r,
    fp_s, fp_r, fx_s, fx_r, b_s, b_r,
    st_s, st_r, dc_s, dc_r,
    mp_s, mp_r, mx_s, mx_r, w_s,
):
    me, col = lax.axis_index("ep"), lax.axis_index("tp")
    partner = col + 1 - 2 * (col % 2)
    across = (col + 2) % tp
    diagonal = (partner + 2) % tp
    tokens, quarter = out2.shape
    slots = disp.shape[0]
    cap = slots // ep
    group = min(GROUP_ROWS, slots)
    per_group = group // cap
    groups = slots // group
    length = q_ref.shape[0]
    chunks = length // CHUNK
    values = v_ref.shape[1] // 2
    rows_out = out1.shape[0]

    def remote(src, dst, s, r, **where):
        return pltpu.make_async_remote_copy(
            src_ref=src, dst_ref=dst, send_sem=s, recv_sem=r, device_id=where, device_id_type=MESH
        )

    loads = [
        pltpu.make_async_copy(a, b, w_s.at[n])
        for n, (a, b) in enumerate(((wg_hbm.at[0], wg), (wu_hbm.at[0], wu), (wd_hbm.at[0], wd), (wo_hbm, wo)))
    ]
    for load in loads:
        load.start()

    barrier = pltpu.get_barrier_semaphore()
    for d in range(1, ep):
        pl.semaphore_signal(barrier, inc=1, device_id={"ep": flip(me, d, ep)}, device_id_type=MESH)
    for peer in (partner, across):
        pl.semaphore_signal(barrier, inc=1, device_id={"tp": peer}, device_id_type=MESH)

    lower = (iota((tokens, tokens), 0) <= iota((tokens, tokens), 1)).astype(BF)
    expert = iota((ep, tokens), 0)
    first_slot = flip(expert, me, ep) * cap - 1
    before = jnp.zeros((ep, 1), F32)
    for choice in range(2):
        named = expert == routes_ref[choice : choice + 1, :]
        rank = dot(named.astype(F32).astype(BF), lower) + before
        place = jnp.sum(jnp.where(named, rank.astype(jnp.int32) + first_slot, 0), axis=0, keepdims=True)
        before = rank[:, tokens - 1 : tokens]
        hot[choice] = (iota((slots, tokens), 0) == place).astype(F32).astype(BF)
    rows = x_ref[...].astype(F32)
    scale = lax.rsqrt(jnp.mean(rows * rows, axis=-1, keepdims=True) + EPS)
    columns = pl.ds(pl.multiple_of(col * quarter, quarter), quarter)
    normed = (x_ref[:, columns].astype(F32) * scale * xgain_ref[:, columns]).astype(BF)
    for g in range(groups):
        span = pl.ds(g * group, group)
        disp[span, :] = dot(hot[0, span, :] + hot[1, span, :], normed).astype(BF)
    recv[col, pl.ds(0, cap), :] = disp[0:cap, :]

    pl.semaphore_wait(barrier, ep + 1)

    def block(d):
        return pl.ds(d * cap, cap)

    def to_expert(d):
        return remote(disp.at[block(d)], recv.at[col, block(d)], ep_s.at[d], ep_r.at[d], ep=flip(me, d, ep))

    def over(d):
        return remote(recv.at[col, block(d)], recv.at[col, block(d)], x_s.at[d], x_r.at[d], tp=across)

    def over_in(d):
        return remote(recv.at[across, block(d)], recv.at[across, block(d)], x_s.at[d], x_r.at[d], tp=across)

    def beside(d):
        return remote(recv.at[col, block(d)], recv.at[col, block(d)], p_s.at[d], p_r.at[d], tp=partner)

    def beside_in(d):
        return remote(recv.at[partner, block(d)], recv.at[partner, block(d)], p_s.at[d], p_r.at[d], tp=partner)

    def relay(d):
        return remote(recv.at[across, block(d)], recv.at[across, block(d)], r_s.at[d], r_r.at[d], tp=partner)

    def relay_in(d):
        return remote(recv.at[diagonal, block(d)], recv.at[diagonal, block(d)], r_s.at[d], r_r.at[d], tp=partner)

    for d in range(1, ep):
        to_expert(d).start()

    def forward(d):
        if d:
            to_expert(d).wait_recv()
        over(d).start()
        beside(d).start()

    def pass_on(d):
        over_in(d).wait_recv()
        relay(d).start()

    forward(0)

    halves = []
    half = CHUNK // 2
    while half:
        halves.append(half)
        half //= 2
    count = len(halves)
    for n, h in enumerate(halves):
        sums[n * CHUNK : (n + 1) * CHUNK, :] = level_sums(h).astype(F32).astype(BF)
    ci, ct = iota((CHUNK, CHUNK), 0), iota((CHUNK, CHUNK), 1)
    sums[count * CHUNK : (count + 1) * CHUNK, :] = (ct <= ci).astype(F32).astype(BF)
    sums[(count + 1) * CHUNK : (count + 2) * CHUNK, :] = (ct > ci).astype(F32).astype(BF)
    width = q_ref.shape[1]
    lane = iota((CHUNK, width), 1)
    head_of = [(lane < width // 2).astype(F32), (lane >= width // 2).astype(F32)]
    ones = jnp.ones((CHUNK, values), BF)
    state[...] = jnp.zeros_like(state)
    so_far = [jnp.zeros((1, width), F32)]

    def recur(c):
        at = pl.ds(c * CHUNK, CHUNK)
        gate = f_ref[at, :].astype(F32)
        log_gate = jnp.minimum(gate, 0.0) - jnp.log1p(jnp.exp(-jnp.abs(gate)))
        extra = jnp.where(lane < width // 2, aux_ref[at, 1:2], aux_ref[at, 2:3])
        decay = log_gate * rate_ref[...] * aux_ref[at, 0:1] + extra
        high = decay.astype(BF)
        low = (decay - high.astype(F32)).astype(BF)
        logs = dot(sums[...], high) + dot(sums[...], low)
        q, k = q_ref[at, :].astype(F32), k_ref[at, :].astype(F32)

        def both(a):
            return jnp.concatenate([a * head_of[0], a * head_of[1]], axis=0).astype(BF)

        def scores(a, b, mask):
            s = dot(both(a), b.astype(BF), ((1,), (1,)))
            return [jnp.where(mask, s[:CHUNK], 0.0), jnp.where(mask, s[CHUNK:], 0.0)]

        total = scores(q, k, ci == ct)
        for n, h in enumerate(halves):
            e = jnp.exp(logs[n * CHUNK : (n + 1) * CHUNK])
            part = scores(q * e, k * e, level_pairs(h))
            total = [total[0] + part[0], total[1] + part[1]]
        prefix = logs[count * CHUNK : (count + 1) * CHUNK]
        suffix = logs[(count + 1) * CHUNK :]
        held = state[...].astype(BF)
        carried = dot(both(q * jnp.exp(prefix)), held)
        key_end = k * jnp.exp(suffix)
        new = jnp.exp(dot(high, ones, ((0,), (0,))) + dot(low, ones, ((0,), (0,)))) * state[...]
        for head in range(2):
            v = v_ref[at, head * values : (head + 1) * values]
            oloc[at, head * values : (head + 1) * values] = (
                dot(total[head].astype(BF), v) + carried[head * CHUNK : (head + 1) * CHUNK]
            )
            new = new + dot((key_end * head_of[head]).astype(BF), v, ((0,), (0,)))
        state[...] = new
        qin[at, :] = (q * jnp.exp(prefix + so_far[0])).astype(BF)
        so_far[0] = so_far[0] + prefix[CHUNK - 1 : CHUNK]

    forwarded, passed = 1, 0
    for c in range(chunks):
        recur(c)
        if c and forwarded < min(ep, 2 * per_group):
            forward(forwarded)
            forwarded += 1
            pass_on(passed)
            passed += 1

    ssend[...] = state[...].astype(BF)
    dsend[...] = jnp.where(iota(dsend.shape, 0) == 0, so_far[0], 0.0)

    def state_out(e):
        return (
            remote(ssend, srecv.at[me], st_s.at[e], st_r.at[me], ep=e),
            remote(dsend, drecv.at[me], dc_s.at[e], dc_r.at[me], ep=e),
        )

    def state_in(e):
        return (
            remote(ssend, srecv.at[e], st_s.at[e], st_r.at[e], ep=e),
            remote(dsend, drecv.at[e], dc_s.at[e], dc_r.at[e], ep=e),
        )

    for e in range(ep):
        @pl.when(e > me)
        def _():
            for copy in state_out(e):
                copy.start()

    def part_copy(g, n):
        at = pl.ds(g * group, group)
        return remote(psend.at[n, at], precv.at[n, at], fp_s.at[n, g], fp_r.at[n, g], tp=partner)

    def sum_copy(g):
        at = pl.ds(g * group, group)
        return remote(xsum.at[at], xrecv.at[at], fx_s.at[g], fx_r.at[g], tp=across)

    def back(d):
        return remote(fin.at[block(d)], ret.at[block(d)], b_s.at[d], b_r.at[d], ep=flip(me, d, ep))

    progress = [forwarded, passed]

    def advance(until, relayed):
        while progress[0] < min(until, ep):
            forward(progress[0])
            progress[0] += 1
        while progress[1] < min(relayed, ep):
            pass_on(progress[1])
            progress[1] += 1

    def experts(g):
        at = pl.ds(g * group, group)
        gate = up = None
        for n in range(tp):
            inner = slice(n * quarter, (n + 1) * quarter)
            piece = recv[n, at, :]
            a, b = dot(piece, wg[inner, :]), dot(piece, wu[inner, :])
            gate, up = (a, b) if gate is None else (gate + a, up + b)
        hidden = (gate * (1.0 / (1.0 + jnp.exp(-gate))) * up).astype(BF)

        def piece_of(c):
            return dot(hidden, wd[:, pl.ds(pl.multiple_of(c * quarter, quarter), quarter)]).astype(BF)

        for n, c in enumerate((diagonal, partner)):
            psend[n, at, :] = piece_of(c)
            part_copy(g, n).start()
        for n, c in enumerate((across, col)):
            pkeep[n, at, :] = piece_of(c)

    def pair(g):
        at = pl.ds(g * group, group)
        part_copy(g, 0).wait_recv()
        xsum[at, :] = (pkeep[0, at, :].astype(F32) + precv[0, at, :].astype(F32)).astype(BF)
        sum_copy(g).start()

    def finish(g):
        at = pl.ds(g * group, group)
        part_copy(g, 1).wait_recv()
        sum_copy(g).wait_recv()
        value = (
            pkeep[1, at, :].astype(F32) + precv[1, at, :].astype(F32) + xrecv[at, :].astype(F32)
        ).astype(BF)
        fin[at, :] = value
        if g == 0:
            ret[0:cap, :] = value[0:cap]
        for d in range(max(1, g * per_group), (g + 1) * per_group):
            back(d).start()

    def mixer_copy(n):
        return remote(msend.at[n], mprecv.at[n], mp_s.at[n], mp_r.at[n], tp=partner)

    def mixer_sum():
        return remote(mxsum, mxrecv, mx_s.at[0], mx_r.at[0], tp=across)

    def mixer_project():
        state[...] = jnp.zeros_like(state)
        for e in range(ep - 1):
            @pl.when(e < me)
            def _():
                for copy in state_in(e):
                    copy.wait_recv()
                logs = lax.dot_general(
                    drecv[e], jnp.ones(drecv.shape[1:2] + (values,), F32), (((0,), (0,)), ((), ())),
                    precision=lax.Precision.HIGHEST, preferred_element_type=F32,
                )
                state[...] = jnp.exp(logs) * state[...] + srecv[e].astype(F32)
        held = state[...]
        row = iota(held.shape, 0)
        for head in range(2):
            mine = (row < width // 2) if head == 0 else (row >= width // 2)
            cols = slice(head * values, (head + 1) * values)
            o = oloc[:, cols] + dot(qin[...], jnp.where(mine, held, 0.0).astype(BF))
            s = lax.rsqrt(jnp.mean(o * o, axis=-1, keepdims=True) + EPS)
            hn[:, cols] = (o * s * hgain_ref[head : head + 1, :]).astype(BF)
        loads[3].wait()

        def piece_of(r):
            return dot(hn[pl.ds(pl.multiple_of(r * rows_out, rows_out), rows_out), :], wo[...]).astype(BF)

        for n, r in enumerate((diagonal, partner)):
            msend[n] = piece_of(r)
            mixer_copy(n).start()
        for n, r in enumerate((across, col)):
            mkeep[n] = piece_of(r)

    def mixer_pair():
        mixer_copy(0).wait_recv()
        mxsum[...] = (mkeep[0].astype(F32) + mprecv[0].astype(F32)).astype(BF)
        mixer_sum().start()

    for load in loads[:3]:
        load.wait()
    for g in range(groups):
        first, last = g * per_group, (g + 1) * per_group
        advance(last, last)
        for d in range(first, last):
            beside_in(d).wait_recv()
            relay_in(d).wait_recv()
        experts(g)
        advance(last + per_group, last)
        pair(g)
        if g:
            finish(g - 1)
        if g == min(2, groups - 1):
            mixer_project()
    mixer_pair()
    finish(groups - 1)

    mixer_copy(1).wait_recv()
    mixer_sum().wait_recv()
    out1[...] = (mkeep[1].astype(F32) + mprecv[1].astype(F32) + mxrecv[...].astype(F32)).astype(BF)

    for d in range(1, ep):
        back(d).wait_recv()
    picked = [dot(hot[choice], ret[...], ((0,), (0,))) for choice in range(2)]
    out2[...] = (picked[0] * w_ref[:, 0:1] + picked[1] * w_ref[:, 1:2]).astype(BF)

    for d in range(ep):
        if d:
            to_expert(d).wait_send()
            back(d).wait_send()
        over(d).wait_send()
        beside(d).wait_send()
        relay(d).wait_send()
    for g in range(groups):
        for n in range(2):
            part_copy(g, n).wait_send()
        sum_copy(g).wait_send()
    for n in range(2):
        mixer_copy(n).wait_send()
    mixer_sum().wait_send()
    for e in range(ep):
        @pl.when(e > me)
        def _():
            for copy in state_out(e):
                copy.wait_send()


def body(q, k, v, f, rate, factor, extra, head_gain, wo, x, x_gain, routes, weights, wg, wu, wd):
    ep, tp = lax.axis_size("ep"), lax.axis_size("tp")
    length, width = q.shape
    values = head_gain.shape[1]
    tokens, model = x.shape
    quarter = model // tp
    hidden = wg.shape[2]
    cap = 4 * tokens // ep
    slots = ep * cap
    group = min(GROUP_ROWS, slots)
    groups = slots // group
    rows_out = length // tp
    aux = jnp.concatenate([factor[:, None], extra], axis=1)
    vm, hbm = pl.BlockSpec(memory_space=pltpu.VMEM), pl.BlockSpec(memory_space=pl.ANY)
    V = pltpu.VMEM
    sem = lambda *shape: pltpu.SemaphoreType.DMA(shape)
    levels = CHUNK.bit_length() + 1
    return pl.pallas_call(
        functools.partial(kernel, ep, tp),
        out_shape=(
            jax.ShapeDtypeStruct((rows_out, model), BF),
            jax.ShapeDtypeStruct((tokens, quarter), BF),
        ),
        in_specs=[vm] * 11 + [hbm] * 4,
        out_specs=(vm, vm),
        scratch_shapes=[
            V((slots, quarter), BF), V((tp, slots, quarter), BF), V((2, slots, quarter), BF),
            V((2, slots, quarter), BF), V((2, slots, quarter), BF), V((slots, quarter), BF),
            V((slots, quarter), BF), V((slots, quarter), BF), V((slots, quarter), BF),
            V((2, slots, tokens), BF),
            V((levels * CHUNK, CHUNK), BF), V((length, 2 * values), F32), V((length, width), BF),
            V((width, values), F32), V((width, values), BF), V((ep, width, values), BF),
            V((8, width), F32), V((ep, 8, width), F32), V((length, 2 * values), BF),
            V((2, rows_out, model), BF), V((2, rows_out, model), BF), V((2, rows_out, model), BF),
            V((rows_out, model), BF), V((rows_out, model), BF),
            V(wo.shape, BF), V(wg.shape[1:], BF), V(wu.shape[1:], BF), V(wd.shape[1:], BF),
            sem(ep), sem(ep), sem(ep), sem(ep), sem(ep), sem(ep), sem(ep), sem(ep),
            sem(2, groups), sem(2, groups), sem(groups), sem(groups), sem(ep), sem(ep),
            sem(ep), sem(ep), sem(ep), sem(ep),
            sem(2), sem(2), sem(1), sem(1), sem(4),
        ],
        compiler_params=pltpu.CompilerParams(
            collective_id=0, has_side_effects=True, vmem_limit_bytes=60 * 1024 * 1024
        ),
    )(q, k, v, f, rate[None], aux, head_gain, x, x_gain[None], routes.T, weights, wo, wg, wu, wd)


def solution(mesh):
    return jax.shard_map(
        body,
        mesh=mesh,
        in_specs=(
            P("ep", "tp"),
            P("ep", "tp"),
            P("ep", "tp"),
            P("ep", "tp"),
            P("tp"),
            P("ep"),
            P("ep", "tp"),
            P("tp", None),
            P("tp", None),
            P("ep", None),
            P(),
            P("ep", None),
            P("ep", None),
            P("ep", None, "tp"),
            P("ep", None, "tp"),
            P("ep", "tp", None),
        ),
        out_specs=(P(("ep", "tp"), None), P("ep", "tp")),
        check_vma=False,
    )
```
